32 devices in a mesh: st: 16 (over z, y, x), tp: 2 (over core).
Axes of the slice: x: 2, y: 2, z: 4, core: 2. Of those that a mesh axis runs over, the one named last changes fastest.
Arguments:
- tokens: bfloat16 [12288, 2048], P('st'), may hold values from -6 to 6, as said below
- route_ids: int32 [192, 4], P('st'), may hold values from 0 to 383, as said below
- store: bfloat16 [384, 128, 2048], P('st'), may hold values from -6 to 6, as said below
- token_gain: float32 [2048], replicated, may hold values from 0.1 to 1.9
- store_gain: float32 [2048], replicated, may hold values from 0.1 to 1.9
- carry_weight: bfloat16 [2048, 512], P(None, 'tp'), may hold values from -0.125 to 0.125
- spatial_weight: bfloat16 [2048, 512], P(None, 'tp'), may hold values from -0.125 to 0.125
- spatial_gain: float32 [512], P('tp'), may hold values from 0.1 to 1.9
- position_mix: bfloat16 [8, 128, 128], P('tp'), may hold values from -0.5 to 0.5
- position_bias: float32 [8, 128], P('tp'), may hold values from 0.1 to 1.9
- query_weight: bfloat16 [2048, 512], P(None, 'tp'), may hold values from -0.86178639 to 0.86178639, as said below
- key_weight: bfloat16 [2048, 512], P(None, 'tp'), may hold values from -0.86178639 to 0.86178639, as said below
- read_weight: bfloat16 [2048, 512], P(None, 'tp'), may hold values from -0.125 to 0.125
- blend_weight: bfloat16 [2048, 512], P(None, 'tp'), may hold values from -0.125 to 0.125
- output_weight: bfloat16 [512, 2048], replicated, may hold values from -0.25 to 0.25
Outputs:
- mixed: bfloat16 [12288, 2048], P(('st', 'tp'))
The draws below stay inside these ranges and needn't reach their ends.
Inputs may be any that keep to these rules, and one draw needn't show every extreme that they name: `route_ids`: each entry is a passage index; passage p is held by index p // 24 of st. All entries of the spans of one index of st (aligned blocks of 12 rows) are different; they name at most 6 passage held by any one index of st, exactly 6 held by the index before their own (cyclically), and at least one held by the index half the axis away. `tokens`: Activations; in some draws the first token of some spans equals a row of a passage that the span reads. `store`: passage rows. `query_weight`: A projection matrix. `key_weight`: A projection matrix.
All inputs are finite; a program needn't handle non-finite values.
Results may differ from the reference program's by a relative error of at most 0.012.
The reference program's roundings to bfloat16 on the way count: a program that leaves them out, or rounds other values in their place, can miss the bound.
Values may be sent and summed in bfloat16 or wider, within the bound.
A program may use at most 128 MiB of HBM per device.

```python
import jax
import jax.numpy as jnp
from jax import lax

D = 2048
HEADS = 8
HEAD_DIM = 64
WIDTH = 512
BLOCK = 128
SPAN = 64
PICKS = 4
PASS_ROWS = 128
PASS_DEV = 24
TOK_DEV = 768
TOKENS = 12288
PASSAGES = 384
CAP = 6
N_ST = 16


def store_passage(key, passage):
    passage_key = jax.random.fold_in(jax.random.fold_in(key, 5), passage)
    sample = jax.random.normal(passage_key, (PASS_ROWS, D), jnp.float32)
    return jnp.clip(sample, -6.0, 6.0)


def draw_store(key, part):
    indices = jnp.arange(PASSAGES, dtype=jnp.int32)
    return lax.map(lambda passage: store_passage(key, passage).astype(jnp.bfloat16), indices)


def route_table(key):
    base_key = jax.random.fold_in(key, 3)
    span_dev = TOK_DEV // SPAN
    wanted = span_dev * PICKS
    pool_size = N_ST * CAP
    ranks = jax.random.permutation(jax.random.fold_in(base_key, 0), N_ST)
    heat = 1 + ranks % 4
    slots = jnp.arange(pool_size, dtype=jnp.int32)
    slot_owner = slots // CAP
    slot_copy = slots % CAP

    def reader(index):
        subkeys = jax.random.split(jax.random.fold_in(base_key, index + 1), 3)
        raw_score = jax.random.randint(subkeys[0], (pool_size,), 0, 4096, dtype=jnp.int32)
        score = raw_score * heat[slot_owner] * pool_size + slots
        before = (index + N_ST - 1) % N_ST
        across = (index + N_ST // 2) % N_ST
        forced = (slot_owner == before) | (slot_owner == across) & (slot_copy == 0)
        score = jnp.where(forced, slots - pool_size, score)
        chosen = jnp.argsort(score)[:wanted]
        owner_index = slot_owner[chosen]
        offset = jax.random.randint(subkeys[1], (N_ST,), 0, PASS_DEV, dtype=jnp.int32)
        passage = owner_index * PASS_DEV + (offset[owner_index] + slot_copy[chosen]) % PASS_DEV
        shuffle = jax.random.permutation(subkeys[2], wanted)
        return passage[shuffle].reshape(span_dev, PICKS)
    table = lax.map(reader, jnp.arange(N_ST, dtype=jnp.int32))
    return table.reshape(N_ST * span_dev, PICKS).astype(jnp.int32)


def draw_route_ids(key, part):
    return route_table(key)


def draw_tokens(key, part):
    sample = jnp.clip(jax.random.normal(jax.random.fold_in(key, 9), (TOKENS, D), jnp.float32), -6.0, 6.0)
    return sample.astype(jnp.bfloat16)


def query_key_pair(key):
    base_key = jax.random.fold_in(key, 13)
    first = jnp.clip(jax.random.normal(jax.random.fold_in(base_key, 0), (D, WIDTH), jnp.float32), -6.0, 6.0)
    second = jnp.clip(jax.random.normal(jax.random.fold_in(base_key, 1), (D, WIDTH), jnp.float32), -6.0, 6.0)
    first = first * D ** (-0.5)
    second = second * D ** (-0.5)
    return (first, second)


def draw_query_weight(key, part):
    return query_key_pair(key)[0].astype(jnp.bfloat16)


def draw_key_weight(key, part):
    return query_key_pair(key)[1].astype(jnp.bfloat16)


def level_of(rng, dims, cuts, least, high):
    factor_of, own = 1.0, jax.random.fold_in(rng, 6)
    for position, blocks in cuts:
        heights = jnp.exp(jax.random.uniform(jax.random.fold_in(own, position), (blocks,), jnp.float32, least / len(cuts), high / len(cuts)))
        factor_of = factor_of * jnp.repeat(heights, dims[position] // blocks).reshape([-1 if axis == position else 1 for axis in range(len(dims))])
    return factor_of


def noise(rng, extent, deviation, most, cuts=(), held_as=jnp.bfloat16):
    drawn = jax.random.normal(rng, extent, jnp.float32) * deviation
    if len(cuts) > 0:
        drawn = level_of(rng, extent, cuts, -0.22, 0.18) * drawn
    return jnp.clip(drawn, min=-most, max=most).astype(held_as)


def setup_inputs(seed: int = 0) -> dict:
    streams_of = jax.random.split(jax.random.key(seed), 16)
    tokens = draw_tokens(jax.random.fold_in(streams_of[15], 71), 0)
    route_ids = draw_route_ids(jax.random.fold_in(streams_of[15], 71), 0)
    store = draw_store(jax.random.fold_in(streams_of[15], 71), 0)
    token_gain = jnp.clip(1.0 + 0.18 * jax.random.normal(streams_of[3], (D,), jnp.float32), 0.1, 1.9)
    store_gain = jnp.clip(1.0 + 0.18 * jax.random.normal(streams_of[4], (D,), jnp.float32), 0.1, 1.9)
    carry_weight = noise(streams_of[5], (D, WIDTH), D ** -0.5, 0.125, ((1, 2),))
    spatial_weight = noise(streams_of[6], (D, WIDTH), D ** -0.5, 0.125, ((1, 2),))
    spatial_gain = jnp.clip(1.0 + 0.18 * jax.random.normal(streams_of[7], (WIDTH,), jnp.float32), 0.1, 1.9)
    position_mix = noise(streams_of[8], (HEADS, BLOCK, BLOCK), BLOCK ** -0.5, 0.5, ((0, 2),))
    position_bias = jnp.clip(1.0 + 0.18 * jax.random.normal(streams_of[9], (HEADS, BLOCK), jnp.float32), 0.1, 1.9)
    query_weight = draw_query_weight(jax.random.fold_in(streams_of[15], 71), 0)
    key_weight = draw_key_weight(jax.random.fold_in(streams_of[15], 71), 0)
    read_weight = noise(streams_of[12], (D, WIDTH), D ** -0.5, 0.125, ((1, 2),))
    blend_weight = noise(streams_of[13], (D, WIDTH), D ** -0.5, 0.125, ((1, 2),))
    output_weight = noise(streams_of[14], (WIDTH, D), WIDTH ** -0.5, 0.25)
    return dict(tokens=tokens, route_ids=route_ids, store=store, token_gain=token_gain, store_gain=store_gain, carry_weight=carry_weight, spatial_weight=spatial_weight, spatial_gain=spatial_gain, position_mix=position_mix, position_bias=position_bias, query_weight=query_weight, key_weight=key_weight, read_weight=read_weight, blend_weight=blend_weight, output_weight=output_weight)


norm_eps = 1e-06

def rms_scaled(matrix, gain_vector):
    values = matrix.astype(jnp.float32)
    scaled = values * lax.rsqrt(lax.optimization_barrier(jnp.mean(values * values, axis=-1, keepdims=True)) + norm_eps)
    return (scaled * gain_vector.astype(jnp.float32)).astype(jnp.bfloat16)

def passage_partial(queries, key_rows, value_rows):
    score_scale = queries.shape[-1] ** (-0.5)
    scores = jnp.einsum('bthe,bplhe->bpthl', queries.astype(jnp.float32), key_rows.astype(jnp.float32)) * score_scale
    score_peak = lax.optimization_barrier(jnp.max(scores, axis=-1, keepdims=True))
    weights = jnp.exp(scores - score_peak)
    weight_total = lax.optimization_barrier(jnp.sum(weights, axis=-1))
    rounded = lax.optimization_barrier(weights.astype(jnp.bfloat16)).astype(jnp.float32)
    summed = jnp.einsum('bpthl,bplhe->bpthe', rounded, value_rows.astype(jnp.float32))
    partial_value = (summed / weight_total[..., None]).astype(jnp.bfloat16)
    return (partial_value, score_peak[..., 0] + jnp.log(weight_total))

def merge_partials(partial_value, log_total):
    level_top = lax.optimization_barrier(jnp.max(log_total, axis=1, keepdims=True))
    weights = jnp.exp(log_total - level_top)
    weight_total = lax.optimization_barrier(jnp.sum(weights, axis=1))
    summed = lax.optimization_barrier(jnp.sum(weights[..., None] * partial_value.astype(jnp.float32), axis=1))
    return summed / weight_total[..., None]

def reference(tokens, route_ids, store, token_gain, store_gain, carry_weight, spatial_weight, spatial_gain, position_mix, position_bias, query_weight, key_weight, read_weight, blend_weight, output_weight):
    row_count = tokens.shape[0]
    normed = rms_scaled(tokens, token_gain)
    carry_branch = jnp.dot(normed, carry_weight, preferred_element_type=jnp.float32)
    spatial = jax.nn.gelu(jnp.dot(normed, spatial_weight, preferred_element_type=jnp.float32), approximate=False)
    channel_mean = lax.optimization_barrier(jnp.mean(spatial, axis=-1, keepdims=True))
    channel_spread = lax.optimization_barrier(jnp.mean(spatial * spatial, axis=-1, keepdims=True)) - channel_mean * channel_mean
    spatial_in = ((spatial - channel_mean) * lax.rsqrt(channel_spread + norm_eps) * spatial_gain.astype(jnp.float32)).astype(jnp.bfloat16)
    blocks = spatial_in.reshape(row_count // BLOCK, BLOCK, HEADS, HEAD_DIM)
    mixed_blocks = jnp.einsum('hij,njhc->nihc', position_mix.astype(jnp.float32), blocks.astype(jnp.float32))
    mixed_blocks = mixed_blocks + position_bias.astype(jnp.float32).T[None, :, :, None]
    gated_mix = jax.nn.gelu(carry_branch, approximate=False) * mixed_blocks.reshape(row_count, HEADS * HEAD_DIM)

    def project(passage):
        passage_normed = rms_scaled(passage, store_gain)
        return (jnp.dot(passage_normed, key_weight, preferred_element_type=jnp.float32).astype(jnp.bfloat16), jnp.dot(passage_normed, read_weight, preferred_element_type=jnp.float32).astype(jnp.bfloat16))
    store_keys, store_values = lax.map(project, store)
    store_keys = store_keys.reshape(store.shape[0], PASS_ROWS, HEADS, HEAD_DIM)
    store_values = store_values.reshape(store.shape[0], PASS_ROWS, HEADS, HEAD_DIM)
    queries = jnp.dot(normed, query_weight, preferred_element_type=jnp.float32).astype(jnp.bfloat16)
    queries = queries.reshape(row_count // SPAN, SPAN, HEADS, HEAD_DIM)

    def attend(item):
        span_queries, picked = item
        span_keys = store_keys[picked][None]
        span_values = store_values[picked][None]
        partial_value, log_total = passage_partial(span_queries[None], span_keys, span_values)
        return merge_partials(partial_value, log_total)[0]
    memory = lax.map(attend, (queries, route_ids)).reshape(row_count, HEADS * HEAD_DIM)
    blend_gate = jax.nn.sigmoid(jnp.dot(normed, blend_weight, preferred_element_type=jnp.float32))
    mixed_rows = (gated_mix + blend_gate * memory).astype(jnp.bfloat16)
    return jnp.dot(mixed_rows, output_weight, preferred_element_type=jnp.float32).astype(jnp.bfloat16)
```

```python
import functools

import jax
import jax.numpy as jnp
from jax import lax
from jax.experimental import pallas as pl
from jax.experimental.pallas import tpu as pltpu
from jax.sharding import PartitionSpec as P

norm_eps = 1e-06
bf16 = jnp.bfloat16
f32 = jnp.float32


def normed_rows(matrix, gain):
    values = matrix.astype(f32)
    scaled = values * lax.rsqrt(jnp.mean(values * values, axis=-1, keepdims=True) + norm_eps)
    return (scaled * gain).astype(bf16)


def query_kernel(span_length, slots, slot_span, tok_ref, gain_ref, wq_ref, normed_ref, sent_ref, q_ref):
    step = pl.program_id(0)
    rows = tok_ref.shape[0]
    normed = normed_rows(tok_ref[...], gain_ref[...])
    normed_ref[...] = normed
    q = jnp.dot(normed, wq_ref[...], preferred_element_type=f32).astype(bf16)
    per = rows // span_length
    for s in range(per):
        q_ref[step * per + s] = q[s * span_length : (s + 1) * span_length]

    @pl.when(step == pl.num_programs(0) - 1)
    def _():
        def body(i, carry):
            sent_ref[i] = q_ref[slot_span[i]]
            return carry

        lax.fori_loop(0, slots, body, 0)


def store_kernel(st_ref, gain_ref, wk_ref, wv_ref, k_ref, vt_ref):
    count, length, _ = st_ref.shape
    for p in range(count):
        normed = normed_rows(st_ref[p], gain_ref[...])
        k_ref[p] = jnp.dot(normed, wk_ref[...], preferred_element_type=f32).astype(bf16)
        v = jnp.dot(normed, wv_ref[...], preferred_element_type=f32)
        vt_ref[p] = v.T.astype(bf16)


def attend(q, k, vt, heads):
    length, width = q.shape
    dim = width // heads
    row_head = lax.broadcasted_iota(jnp.int32, (heads * length, width), 0) // length
    lane_head = lax.broadcasted_iota(jnp.int32, (heads * length, width), 1) // dim
    stacked = jnp.where(row_head == lane_head, jnp.concatenate([q] * heads, axis=0), jnp.zeros((), bf16))
    s = lax.dot_general(k, stacked, (((1,), (1,)), ((), ())), preferred_element_type=f32) * dim ** (-0.5)
    peak = jnp.max(s, axis=0, keepdims=True)
    w = jnp.exp(s - peak)
    total = jnp.sum(w, axis=0, keepdims=True)
    o = jnp.dot(vt, w.astype(bf16), preferred_element_type=f32)
    col_head = lax.broadcasted_iota(jnp.int32, (dim, heads * length), 1) // length
    out = o[0:dim]
    for h in range(1, heads):
        out = jnp.where(col_head == h, o[h * dim : (h + 1) * dim], out)
    return (out / total).astype(bf16), peak + jnp.log(total)


def attention_kernel(heads, ids, q_ref, k_ref, vt_ref, val_ref, lev_ref):
    src = pl.program_id(0)
    cap = q_ref.shape[1]
    for c in range(cap):
        i = ids[src * cap + c]
        val, lev = attend(q_ref[0, c], k_ref[i], vt_ref[i], heads)
        val_ref[0, c] = val
        lev_ref[0, c] = lev


def merge_kernel(heads, spans, picks, pos, val_ref, lev_ref, gated_ref, blend_ref, out_ref):
    step = pl.program_id(0)
    dim, width = val_ref.shape[1:]
    length = width // heads
    for s in range(spans):
        first = (step * spans + s) * picks
        levels = [lev_ref[pos[first + p]] for p in range(picks)]
        top = functools.reduce(jnp.maximum, levels)
        ws = [jnp.exp(lev - top) for lev in levels]
        total = sum(ws)
        summed = sum(w * val_ref[pos[first + p]].astype(f32) for p, w in enumerate(ws))
        mem = (summed / total).T
        mem = jnp.concatenate([mem[h * length : (h + 1) * length] for h in range(heads)], axis=1)
        rows = slice(s * length, (s + 1) * length)
        out_ref[rows] = (gated_ref[rows] + blend_ref[rows] * mem).astype(bf16)


def per_device(
    tokens,
    route_ids,
    store,
    token_gain,
    store_gain,
    carry_weight,
    spatial_weight,
    spatial_gain,
    position_mix,
    position_bias,
    query_weight,
    key_weight,
    read_weight,
    blend_weight,
    output_weight,
):
    row_count, model = tokens.shape
    local_heads, block_length = position_mix.shape[:2]
    width = carry_weight.shape[1]
    head_dim = width // local_heads
    span_count, pick_count = route_ids.shape
    span_length = row_count // span_count
    store_count, passage_length = store.shape[:2]
    owner_count = lax.axis_size("st")
    requests = span_count * pick_count
    cap = max(1, 2 * requests // owner_count)
    slots = owner_count * cap

    flat_ids = route_ids.reshape(requests)
    owner = flat_ids // store_count
    order = jnp.arange(requests, dtype=jnp.int32)
    earlier = (owner[:, None] == owner[None, :]) & (order[None, :] < order[:, None])
    position = owner * cap + jnp.sum(earlier.astype(jnp.int32), axis=1)
    hit = position[None, :] == jnp.arange(slots, dtype=jnp.int32)[:, None]
    slot_local = jnp.sum(jnp.where(hit, (flat_ids % store_count)[None, :], 0), axis=1)
    slot_span = jnp.sum(jnp.where(hit, (order // pick_count)[None, :], 0), axis=1)
    piece_local = lax.all_to_all(
        slot_local.reshape(owner_count, cap), "st", split_axis=0, concat_axis=0, tiled=True
    ).reshape(slots)

    tile = 2 * span_length
    normed, sent = pl.pallas_call(
        functools.partial(query_kernel, span_length, slots),
        grid_spec=pltpu.PrefetchScalarGridSpec(
            num_scalar_prefetch=1,
            grid=(row_count // tile,),
            in_specs=[
                pl.BlockSpec((tile, model), lambda i, _: (i, 0)),
                pl.BlockSpec((1, model), lambda i, _: (0, 0)),
                pl.BlockSpec((model, width), lambda i, _: (0, 0)),
            ],
            out_specs=[
                pl.BlockSpec((tile, model), lambda i, _: (i, 0)),
                pl.BlockSpec((slots, span_length, width), lambda i, _: (0, 0, 0)),
            ],
            scratch_shapes=[pltpu.VMEM((span_count, span_length, width), bf16)],
        ),
        out_shape=[
            jax.ShapeDtypeStruct((row_count, model), bf16),
            jax.ShapeDtypeStruct((slots, span_length, width), bf16),
        ],
        cost_estimate=pl.CostEstimate(
            flops=2 * row_count * model * width, bytes_accessed=4 * row_count * model, transcendentals=0
        ),
        name="query",
    )(slot_span, tokens, token_gain.reshape(1, model), query_weight)
    piece_q = lax.all_to_all(
        sent.reshape(owner_count, cap, span_length, width), "st", split_axis=0, concat_axis=0, tiled=True
    )

    group = 2
    keys, values_t = pl.pallas_call(
        store_kernel,
        grid=(store_count // group,),
        in_specs=[
            pl.BlockSpec((group, passage_length, model), lambda i: (i, 0, 0)),
            pl.BlockSpec((1, model), lambda i: (0, 0)),
            pl.BlockSpec((model, width), lambda i: (0, 0)),
            pl.BlockSpec((model, width), lambda i: (0, 0)),
        ],
        out_specs=[
            pl.BlockSpec((group, passage_length, width), lambda i: (i, 0, 0)),
            pl.BlockSpec((group, width, passage_length), lambda i: (i, 0, 0)),
        ],
        out_shape=[
            jax.ShapeDtypeStruct((store_count, passage_length, width), bf16),
            jax.ShapeDtypeStruct((store_count, width, passage_length), bf16),
        ],
        cost_estimate=pl.CostEstimate(
            flops=4 * store_count * passage_length * model * width,
            bytes_accessed=2 * store_count * passage_length * model,
            transcendentals=0,
        ),
        name="store",
    )(store, store_gain.reshape(1, model), key_weight, read_weight)

    part_values, part_levels = pl.pallas_call(
        functools.partial(attention_kernel, local_heads),
        grid_spec=pltpu.PrefetchScalarGridSpec(
            num_scalar_prefetch=1,
            grid=(owner_count,),
            in_specs=[
                pl.BlockSpec((1, cap, span_length, width), lambda i, _: (i, 0, 0, 0)),
                pl.BlockSpec((store_count, passage_length, width), lambda i, _: (0, 0, 0)),
                pl.BlockSpec((store_count, width, passage_length), lambda i, _: (0, 0, 0)),
            ],
            out_specs=[
                pl.BlockSpec((1, cap, head_dim, local_heads * span_length), lambda i, _: (i, 0, 0, 0)),
                pl.BlockSpec((1, cap, 1, local_heads * span_length), lambda i, _: (i, 0, 0, 0)),
            ],
        ),
        out_shape=[
            jax.ShapeDtypeStruct((owner_count, cap, head_dim, local_heads * span_length), bf16),
            jax.ShapeDtypeStruct((owner_count, cap, 1, local_heads * span_length), f32),
        ],
        name="attention",
    )(piece_local, piece_q, keys, values_t)
    back_values = lax.all_to_all(part_values, "st", split_axis=0, concat_axis=0, tiled=True)
    back_levels = lax.all_to_all(part_levels, "st", split_axis=0, concat_axis=0, tiled=True)

    carry_branch = jnp.dot(normed, carry_weight, preferred_element_type=f32)
    spatial = jax.nn.gelu(jnp.dot(normed, spatial_weight, preferred_element_type=f32), approximate=False)
    total_width = width * lax.axis_size("tp")
    moment_one, moment_two = lax.psum(
        (jnp.sum(spatial, axis=1), jnp.sum(spatial * spatial, axis=1)), "tp"
    )
    channel_mean = (moment_one / total_width)[:, None]
    channel_spread = (moment_two / total_width)[:, None] - channel_mean * channel_mean
    spatial_in = (
        (spatial - channel_mean) * lax.rsqrt(channel_spread + norm_eps) * spatial_gain
    ).astype(bf16)
    blocks = spatial_in.reshape(row_count // block_length, block_length, local_heads, head_dim)
    mixed_blocks = jnp.einsum("hij,njhc->nihc", position_mix, blocks, preferred_element_type=f32)
    mixed_blocks = mixed_blocks + position_bias.T[None, :, :, None]
    gated_mix = jax.nn.gelu(carry_branch, approximate=False) * mixed_blocks.reshape(row_count, width)
    blend_gate = jax.nn.sigmoid(jnp.dot(normed, blend_weight, preferred_element_type=f32))

    spans = 4 if span_count % 4 == 0 else 1
    mixed_rows = pl.pallas_call(
        functools.partial(merge_kernel, local_heads, spans, pick_count),
        grid_spec=pltpu.PrefetchScalarGridSpec(
            num_scalar_prefetch=1,
            grid=(span_count // spans,),
            in_specs=[
                pl.BlockSpec((slots, head_dim, local_heads * span_length), lambda i, _: (0, 0, 0)),
                pl.BlockSpec((slots, 1, local_heads * span_length), lambda i, _: (0, 0, 0)),
                pl.BlockSpec((spans * span_length, width), lambda i, _: (i, 0)),
                pl.BlockSpec((spans * span_length, width), lambda i, _: (i, 0)),
            ],
            out_specs=pl.BlockSpec((spans * span_length, width), lambda i, _: (i, 0)),
        ),
        out_shape=jax.ShapeDtypeStruct((row_count, width), bf16),
        name="merge",
    )(
        position,
        back_values.reshape(slots, head_dim, local_heads * span_length),
        back_levels.reshape(slots, 1, local_heads * span_length),
        gated_mix,
        blend_gate,
    )
    by_rows = lax.all_to_all(mixed_rows, "tp", split_axis=0, concat_axis=1, tiled=True)
    return jnp.dot(by_rows, output_weight, preferred_element_type=f32).astype(bf16)


def solution(mesh):
    in_specs = (
        P("st", None),
        P("st", None),
        P("st", None, None),
        P(),
        P(),
        P(None, "tp"),
        P(None, "tp"),
        P("tp"),
        P("tp", None, None),
        P("tp", None),
        P(None, "tp"),
        P(None, "tp"),
        P(None, "tp"),
        P(None, "tp"),
        P(),
    )
    out_specs = P(("st", "tp"), None)
    return jax.shard_map(
        per_device, mesh=mesh, in_specs=in_specs, out_specs=out_specs, check_vma=False
    )
```

```python
import functools

import jax
import jax.numpy as jnp
from jax import lax
from jax.experimental import pallas as pl
from jax.experimental.pallas import tpu as pltpu
from jax.sharding import PartitionSpec as P

norm_eps = 1e-06
bf16 = jnp.bfloat16
f32 = jnp.float32


def normed_rows(matrix, gain):
    values = matrix.astype(f32)
    scaled = values * lax.rsqrt(jnp.mean(values * values, axis=-1, keepdims=True) + norm_eps)
    return (scaled * gain).astype(bf16)


def query_kernel(span_length, slots, slot_span, tok_ref, gain_ref, wq_ref, normed_ref, sent_ref, q_ref):
    step = pl.program_id(0)
    rows = tok_ref.shape[0]
    normed = normed_rows(tok_ref[...], gain_ref[...])
    normed_ref[...] = normed
    q = jnp.dot(normed, wq_ref[...], preferred_element_type=f32).astype(bf16)
    per = rows // span_length
    for s in range(per):
        q_ref[step * per + s] = q[s * span_length : (s + 1) * span_length]

    @pl.when(step == pl.num_programs(0) - 1)
    def _():
        def body(i, carry):
            sent_ref[i] = q_ref[slot_span[i]]
            return carry

        lax.fori_loop(0, slots, body, 0)


def store_kernel(st_ref, gain_ref, wk_ref, wv_ref, k_ref, vt_ref):
    count, length, _ = st_ref.shape
    for p in range(count):
        normed = normed_rows(st_ref[p], gain_ref[...])
        k_ref[p] = jnp.dot(normed, wk_ref[...], preferred_element_type=f32).astype(bf16)
        v = jnp.dot(normed, wv_ref[...], preferred_element_type=f32)
        vt_ref[p] = v.T.astype(bf16)


def attend(q, k, vt, heads):
    length, width = q.shape
    dim = width // heads
    row_head = lax.broadcasted_iota(jnp.int32, (heads * length, width), 0) // length
    lane_head = lax.broadcasted_iota(jnp.int32, (heads * length, width), 1) // dim
    stacked = jnp.where(row_head == lane_head, jnp.concatenate([q] * heads, axis=0), jnp.zeros((), bf16))
    s = lax.dot_general(k, stacked, (((1,), (1,)), ((), ())), preferred_element_type=f32) * dim ** (-0.5)
    peak = jnp.max(s, axis=0, keepdims=True)
    w = jnp.exp(s - peak)
    total = jnp.sum(w, axis=0, keepdims=True)
    o = jnp.dot(vt, w.astype(bf16), preferred_element_type=f32)
    col_head = lax.broadcasted_iota(jnp.int32, (dim, heads * length), 1) // length
    out = o[0:dim]
    for h in range(1, heads):
        out = jnp.where(col_head == h, o[h * dim : (h + 1) * dim], out)
    return (out / total).astype(bf16), peak + jnp.log(total)


def attention_kernel(heads, n, ids, q_ref, k_ref, vt_ref, val_ref, lev_ref, out_val, out_lev, send, recv):
    me = lax.axis_index("st")
    cap = q_ref.shape[1]

    barrier = pltpu.get_barrier_semaphore()

    def greet(d, carry):
        pl.semaphore_signal(
            barrier,
            inc=1,
            device_id={"st": lax.rem(me + d, n)},
            device_id_type=pl.DeviceIdType.MESH,
        )
        return carry

    lax.fori_loop(1, n, greet, 0)
    pl.semaphore_wait(barrier, n - 1)

    def compute(dst, val_to, lev_to):
        for c in range(cap):
            i = ids[dst * cap + c]
            val, lev = attend(q_ref[dst, c], k_ref[i], vt_ref[i], heads)
            val_to[dst, c] = val
            lev_to[dst, c : c + 1] = lev

    def copies(d):
        dst = lax.rem(me + d, n)
        pairs = ((out_val, val_ref), (out_lev, lev_ref))
        return [
            pltpu.make_async_remote_copy(
                src_ref=src.at[dst],
                dst_ref=to.at[me],
                send_sem=send.at[j, d],
                recv_sem=recv.at[j, d],
                device_id={"st": dst},
                device_id_type=pl.DeviceIdType.MESH,
            )
            for j, (src, to) in enumerate(pairs)
        ]

    def offset(i):
        j = n // 2 + i
        return j % n + j // n

    def launch(d):
        for copy in copies(d):
            copy.start()

    compute(lax.rem(me + offset(0), n), out_val, out_lev)

    def step(i, carry):
        compute(lax.rem(me + offset(i), n), out_val, out_lev)
        launch(offset(i - 1))
        return carry

    lax.fori_loop(1, n - 1, step, 0)
    compute(me, val_ref, lev_ref)
    launch(offset(n - 2))

    def finish(d, carry):
        for copy in copies(d):
            copy.wait()
        return carry

    lax.fori_loop(1, n, finish, 0)


def merge_kernel(heads, spans, picks, pos, val_ref, lev_ref, gated_ref, blend_ref, out_ref):
    step = pl.program_id(0)
    dim, width = val_ref.shape[1:]
    length = width // heads
    for s in range(spans):
        first = (step * spans + s) * picks
        levels = [lev_ref[pos[first + p]] for p in range(picks)]
        top = functools.reduce(jnp.maximum, levels)
        ws = [jnp.exp(lev - top) for lev in levels]
        total = sum(ws)
        summed = sum(w * val_ref[pos[first + p]].astype(f32) for p, w in enumerate(ws))
        mem = (summed / total).T
        mem = jnp.concatenate([mem[h * length : (h + 1) * length] for h in range(heads)], axis=1)
        rows = slice(s * length, (s + 1) * length)
        out_ref[rows] = (gated_ref[rows] + blend_ref[rows] * mem).astype(bf16)


def per_device(
    tokens,
    route_ids,
    store,
    token_gain,
    store_gain,
    carry_weight,
    spatial_weight,
    spatial_gain,
    position_mix,
    position_bias,
    query_weight,
    key_weight,
    read_weight,
    blend_weight,
    output_weight,
):
    row_count, model = tokens.shape
    local_heads, block_length = position_mix.shape[:2]
    width = carry_weight.shape[1]
    head_dim = width // local_heads
    span_count, pick_count = route_ids.shape
    span_length = row_count // span_count
    store_count, passage_length = store.shape[:2]
    owner_count = lax.axis_size("st")
    requests = span_count * pick_count
    cap = max(1, 2 * requests // owner_count)
    slots = owner_count * cap

    flat_ids = route_ids.reshape(requests)
    owner = flat_ids // store_count
    order = jnp.arange(requests, dtype=jnp.int32)
    earlier = (owner[:, None] == owner[None, :]) & (order[None, :] < order[:, None])
    position = owner * cap + jnp.sum(earlier.astype(jnp.int32), axis=1)
    hit = position[None, :] == jnp.arange(slots, dtype=jnp.int32)[:, None]
    slot_local = jnp.sum(jnp.where(hit, (flat_ids % store_count)[None, :], 0), axis=1)
    slot_span = jnp.sum(jnp.where(hit, (order // pick_count)[None, :], 0), axis=1)
    piece_local = lax.all_to_all(
        slot_local.reshape(owner_count, cap), "st", split_axis=0, concat_axis=0, tiled=True
    ).reshape(slots)

    tile = 2 * span_length
    normed, sent = pl.pallas_call(
        functools.partial(query_kernel, span_length, slots),
        grid_spec=pltpu.PrefetchScalarGridSpec(
            num_scalar_prefetch=1,
            grid=(row_count // tile,),
            in_specs=[
                pl.BlockSpec((tile, model), lambda i, _: (i, 0)),
                pl.BlockSpec((1, model), lambda i, _: (0, 0)),
                pl.BlockSpec((model, width), lambda i, _: (0, 0)),
            ],
            out_specs=[
                pl.BlockSpec((tile, model), lambda i, _: (i, 0)),
                pl.BlockSpec((slots, span_length, width), lambda i, _: (0, 0, 0)),
            ],
            scratch_shapes=[pltpu.VMEM((span_count, span_length, width), bf16)],
        ),
        out_shape=[
            jax.ShapeDtypeStruct((row_count, model), bf16),
            jax.ShapeDtypeStruct((slots, span_length, width), bf16),
        ],
        cost_estimate=pl.CostEstimate(
            flops=2 * row_count * model * width, bytes_accessed=4 * row_count * model, transcendentals=0
        ),
        name="query",
    )(slot_span, tokens, token_gain.reshape(1, model), query_weight)
    piece_q = lax.all_to_all(
        sent.reshape(owner_count, cap, span_length, width), "st", split_axis=0, concat_axis=0, tiled=True
    )

    group = 2
    keys, values_t = pl.pallas_call(
        store_kernel,
        grid=(store_count // group,),
        in_specs=[
            pl.BlockSpec((group, passage_length, model), lambda i: (i, 0, 0)),
            pl.BlockSpec((1, model), lambda i: (0, 0)),
            pl.BlockSpec((model, width), lambda i: (0, 0)),
            pl.BlockSpec((model, width), lambda i: (0, 0)),
        ],
        out_specs=[
            pl.BlockSpec((group, passage_length, width), lambda i: (i, 0, 0)),
            pl.BlockSpec((group, width, passage_length), lambda i: (i, 0, 0)),
        ],
        out_shape=[
            jax.ShapeDtypeStruct((store_count, passage_length, width), bf16),
            jax.ShapeDtypeStruct((store_count, width, passage_length), bf16),
        ],
        cost_estimate=pl.CostEstimate(
            flops=4 * store_count * passage_length * model * width,
            bytes_accessed=2 * store_count * passage_length * model,
            transcendentals=0,
        ),
        name="store",
    )(store, store_gain.reshape(1, model), key_weight, read_weight)

    carry_branch = jnp.dot(normed, carry_weight, preferred_element_type=f32)
    spatial = jax.nn.gelu(jnp.dot(normed, spatial_weight, preferred_element_type=f32), approximate=False)
    total_width = width * lax.axis_size("tp")
    moment_one, moment_two = lax.psum(
        (jnp.sum(spatial, axis=1), jnp.sum(spatial * spatial, axis=1)), "tp"
    )
    channel_mean = (moment_one / total_width)[:, None]
    channel_spread = (moment_two / total_width)[:, None] - channel_mean * channel_mean
    spatial_in = (
        (spatial - channel_mean) * lax.rsqrt(channel_spread + norm_eps) * spatial_gain
    ).astype(bf16)
    blocks = spatial_in.reshape(row_count // block_length, block_length, local_heads, head_dim)
    mixed_blocks = jnp.einsum("hij,njhc->nihc", position_mix, blocks, preferred_element_type=f32)
    mixed_blocks = mixed_blocks + position_bias.T[None, :, :, None]
    gated_mix = jax.nn.gelu(carry_branch, approximate=False) * mixed_blocks.reshape(row_count, width)
    blend_gate = jax.nn.sigmoid(jnp.dot(normed, blend_weight, preferred_element_type=f32))

    keys, gated_mix, blend_gate = lax.optimization_barrier((keys, gated_mix, blend_gate))
    value_shape = (owner_count, cap, head_dim, local_heads * span_length)
    level_shape = (owner_count, cap, local_heads * span_length)
    vmem = pl.BlockSpec(memory_space=pltpu.VMEM)
    back_values, back_levels = pl.pallas_call(
        functools.partial(attention_kernel, local_heads, owner_count),
        in_specs=[pl.BlockSpec(memory_space=pltpu.SMEM), vmem, vmem, vmem],
        out_specs=[vmem, vmem],
        out_shape=[jax.ShapeDtypeStruct(value_shape, bf16), jax.ShapeDtypeStruct(level_shape, f32)],
        scratch_shapes=[
            pltpu.VMEM(value_shape, bf16),
            pltpu.VMEM(level_shape, f32),
            pltpu.SemaphoreType.DMA((2, owner_count)),
            pltpu.SemaphoreType.DMA((2, owner_count)),
        ],
        compiler_params=pltpu.CompilerParams(collective_id=0, has_side_effects=True),
        name="attention",
    )(piece_local, piece_q, keys, values_t)

    spans = 4 if span_count % 4 == 0 else 1
    mixed_rows = pl.pallas_call(
        functools.partial(merge_kernel, local_heads, spans, pick_count),
        grid_spec=pltpu.PrefetchScalarGridSpec(
            num_scalar_prefetch=1,
            grid=(span_count // spans,),
            in_specs=[
                pl.BlockSpec((slots, head_dim, local_heads * span_length), lambda i, _: (0, 0, 0)),
                pl.BlockSpec((slots, 1, local_heads * span_length), lambda i, _: (0, 0, 0)),
                pl.BlockSpec((spans * span_length, width), lambda i, _: (i, 0)),
                pl.BlockSpec((spans * span_length, width), lambda i, _: (i, 0)),
            ],
            out_specs=pl.BlockSpec((spans * span_length, width), lambda i, _: (i, 0)),
        ),
        out_shape=jax.ShapeDtypeStruct((row_count, width), bf16),
        name="merge",
    )(
        position,
        back_values.reshape(slots, head_dim, local_heads * span_length),
        back_levels.reshape(slots, 1, local_heads * span_length),
        gated_mix,
        blend_gate,
    )
    by_rows = lax.all_to_all(mixed_rows, "tp", split_axis=0, concat_axis=1, tiled=True)
    return jnp.dot(by_rows, output_weight, preferred_element_type=f32).astype(bf16)


def solution(mesh):
    in_specs = (
        P("st", None),
        P("st", None),
        P("st", None, None),
        P(),
        P(),
        P(None, "tp"),
        P(None, "tp"),
        P("tp"),
        P("tp", None, None),
        P("tp", None),
        P(None, "tp"),
        P(None, "tp"),
        P(None, "tp"),
        P(None, "tp"),
        P(),
    )
    out_specs = P(("st", "tp"), None)
    return jax.shard_map(
        per_device, mesh=mesh, in_specs=in_specs, out_specs=out_specs, check_vma=False
    )
```

```python
import functools

import jax
import jax.numpy as jnp
from jax import lax
from jax.experimental import pallas as pl
from jax.experimental.pallas import tpu as pltpu
from jax.sharding import PartitionSpec as P

norm_eps = 1e-06
bf16 = jnp.bfloat16
f32 = jnp.float32


def normed_rows(matrix, gain):
    values = matrix.astype(f32)
    scaled = values * lax.rsqrt(jnp.mean(values * values, axis=-1, keepdims=True) + norm_eps)
    return (scaled * gain).astype(bf16)


def query_kernel(tok_ref, gain_ref, wq_ref, normed_ref, q_ref):
    normed = normed_rows(tok_ref[...], gain_ref[...])
    normed_ref[...] = normed
    q_ref[...] = jnp.dot(normed, wq_ref[...], preferred_element_type=f32).astype(bf16)


def store_kernel(st_ref, gain_ref, wk_ref, wv_ref, k_ref, vt_ref):
    count, length, _ = st_ref.shape
    for p in range(count):
        normed = normed_rows(st_ref[p], gain_ref[...])
        k_ref[p] = jnp.dot(normed, wk_ref[...], preferred_element_type=f32).astype(bf16)
        v = jnp.dot(normed, wv_ref[...], preferred_element_type=f32)
        vt_ref[p] = v.T.astype(bf16)


def attend(q, k, vt, heads):
    length, width = q.shape
    dim = width // heads
    row_head = lax.broadcasted_iota(jnp.int32, (heads * length, width), 0) // length
    lane_head = lax.broadcasted_iota(jnp.int32, (heads * length, width), 1) // dim
    stacked = jnp.where(row_head == lane_head, jnp.concatenate([q] * heads, axis=0), jnp.zeros((), bf16))
    s = lax.dot_general(k, stacked, (((1,), (1,)), ((), ())), preferred_element_type=f32) * dim ** (-0.5)
    peak = jnp.max(s, axis=0, keepdims=True)
    w = jnp.exp(s - peak)
    total = jnp.sum(w, axis=0, keepdims=True)
    o = jnp.dot(vt, w.astype(bf16), preferred_element_type=f32)
    col_head = lax.broadcasted_iota(jnp.int32, (dim, heads * length), 1) // length
    out = o[0:dim]
    for h in range(1, heads):
        out = jnp.where(col_head == h, o[h * dim : (h + 1) * dim], out)
    return (out / total).astype(bf16), peak + jnp.log(total)


def attention_kernel(heads, n, cap, ids, picked, q_ref, k_ref, vt_ref, val_ref, lev_ref, out_val, out_lev, send, recv):
    me = lax.axis_index("st")

    barrier = pltpu.get_barrier_semaphore()

    def greet(d, carry):
        pl.semaphore_signal(
            barrier,
            inc=1,
            device_id={"st": lax.rem(me + d, n)},
            device_id_type=pl.DeviceIdType.MESH,
        )
        return carry

    lax.fori_loop(1, n, greet, 0)
    pl.semaphore_wait(barrier, n - 1)

    def compute(dst, val_to, lev_to):
        for c in range(cap):
            i = ids[dst * cap + c]
            val, lev = attend(q_ref[dst, picked[dst * cap + c]], k_ref[i], vt_ref[i], heads)
            val_to[dst, c] = val
            lev_to[dst, c : c + 1] = lev

    def copies(d):
        dst = lax.rem(me + d, n)
        pairs = ((out_val, val_ref), (out_lev, lev_ref))
        return [
            pltpu.make_async_remote_copy(
                src_ref=src.at[dst],
                dst_ref=to.at[me],
                send_sem=send.at[j, d],
                recv_sem=recv.at[j, d],
                device_id={"st": dst},
                device_id_type=pl.DeviceIdType.MESH,
            )
            for j, (src, to) in enumerate(pairs)
        ]

    def offset(i):
        j = n // 2 + i
        return j % n + j // n

    def launch(d):
        for copy in copies(d):
            copy.start()

    compute(lax.rem(me + offset(0), n), out_val, out_lev)

    def step(i, carry):
        compute(lax.rem(me + offset(i), n), out_val, out_lev)
        launch(offset(i - 1))
        return carry

    lax.fori_loop(1, n - 1, step, 0)
    compute(me, val_ref, lev_ref)
    launch(offset(n - 2))

    def finish(d, carry):
        for copy in copies(d):
            copy.wait()
        return carry

    lax.fori_loop(1, n, finish, 0)


def merge_kernel(heads, spans, picks, pos, val_ref, lev_ref, gated_ref, blend_ref, out_ref):
    step = pl.program_id(0)
    dim, width = val_ref.shape[1:]
    length = width // heads
    for s in range(spans):
        first = (step * spans + s) * picks
        levels = [lev_ref[pos[first + p]] for p in range(picks)]
        top = functools.reduce(jnp.maximum, levels)
        ws = [jnp.exp(lev - top) for lev in levels]
        total = sum(ws)
        summed = sum(w * val_ref[pos[first + p]].astype(f32) for p, w in enumerate(ws))
        mem = (summed / total).T
        mem = jnp.concatenate([mem[h * length : (h + 1) * length] for h in range(heads)], axis=1)
        rows = slice(s * length, (s + 1) * length)
        out_ref[rows] = (gated_ref[rows] + blend_ref[rows] * mem).astype(bf16)


def per_device(
    tokens,
    route_ids,
    store,
    token_gain,
    store_gain,
    carry_weight,
    spatial_weight,
    spatial_gain,
    position_mix,
    position_bias,
    query_weight,
    key_weight,
    read_weight,
    blend_weight,
    output_weight,
):
    row_count, model = tokens.shape
    local_heads, block_length = position_mix.shape[:2]
    width = carry_weight.shape[1]
    head_dim = width // local_heads
    span_count, pick_count = route_ids.shape
    span_length = row_count // span_count
    store_count, passage_length = store.shape[:2]
    owner_count = lax.axis_size("st")
    requests = span_count * pick_count
    cap = max(1, 2 * requests // owner_count)
    slots = owner_count * cap

    flat_ids = route_ids.reshape(requests)
    owner = flat_ids // store_count
    order = jnp.arange(requests, dtype=jnp.int32)
    earlier = (owner[:, None] == owner[None, :]) & (order[None, :] < order[:, None])
    position = owner * cap + jnp.sum(earlier.astype(jnp.int32), axis=1)

    asked = lax.all_gather(flat_ids, "st", axis=0, tiled=False)
    mine = asked // store_count == lax.axis_index("st")
    before = jnp.sum(
        jnp.where(mine[:, None, :] & (order[None, None, :] < order[None, :, None]), 1, 0), axis=2
    )
    hit = mine[:, None, :] & (before[:, None, :] == jnp.arange(cap, dtype=jnp.int32)[None, :, None])
    slot_local = jnp.sum(jnp.where(hit, (asked % store_count)[:, None, :], 0), axis=2).reshape(slots)
    slot_span = jnp.sum(jnp.where(hit, order // pick_count, 0), axis=2).reshape(slots)

    tile = 2 * span_length
    normed, queries = pl.pallas_call(
        query_kernel,
        grid=(row_count // tile,),
        in_specs=[
            pl.BlockSpec((tile, model), lambda i: (i, 0)),
            pl.BlockSpec((1, model), lambda i: (0, 0)),
            pl.BlockSpec((model, width), lambda i: (0, 0)),
        ],
        out_specs=[
            pl.BlockSpec((tile, model), lambda i: (i, 0)),
            pl.BlockSpec((tile, width), lambda i: (i, 0)),
        ],
        out_shape=[
            jax.ShapeDtypeStruct((row_count, model), bf16),
            jax.ShapeDtypeStruct((row_count, width), bf16),
        ],
        cost_estimate=pl.CostEstimate(
            flops=2 * row_count * model * width, bytes_accessed=4 * row_count * model, transcendentals=0
        ),
        name="query",
    )(tokens, token_gain.reshape(1, model), query_weight)
    all_queries = lax.all_gather(
        queries.reshape(span_count, span_length, width), "st", axis=0, tiled=False
    )

    group = 2
    keys, values_t = pl.pallas_call(
        store_kernel,
        grid=(store_count // group,),
        in_specs=[
            pl.BlockSpec((group, passage_length, model), lambda i: (i, 0, 0)),
            pl.BlockSpec((1, model), lambda i: (0, 0)),
            pl.BlockSpec((model, width), lambda i: (0, 0)),
            pl.BlockSpec((model, width), lambda i: (0, 0)),
        ],
        out_specs=[
            pl.BlockSpec((group, passage_length, width), lambda i: (i, 0, 0)),
            pl.BlockSpec((group, width, passage_length), lambda i: (i, 0, 0)),
        ],
        out_shape=[
            jax.ShapeDtypeStruct((store_count, passage_length, width), bf16),
            jax.ShapeDtypeStruct((store_count, width, passage_length), bf16),
        ],
        cost_estimate=pl.CostEstimate(
            flops=4 * store_count * passage_length * model * width,
            bytes_accessed=2 * store_count * passage_length * model,
            transcendentals=0,
        ),
        name="store",
    )(store, store_gain.reshape(1, model), key_weight, read_weight)

    carry_branch = jnp.dot(normed, carry_weight, preferred_element_type=f32)
    spatial = jax.nn.gelu(jnp.dot(normed, spatial_weight, preferred_element_type=f32), approximate=False)
    total_width = width * lax.axis_size("tp")
    moment_one, moment_two = lax.psum(
        (jnp.sum(spatial, axis=1), jnp.sum(spatial * spatial, axis=1)), "tp"
    )
    channel_mean = (moment_one / total_width)[:, None]
    channel_spread = (moment_two / total_width)[:, None] - channel_mean * channel_mean
    spatial_in = (
        (spatial - channel_mean) * lax.rsqrt(channel_spread + norm_eps) * spatial_gain
    ).astype(bf16)
    blocks = spatial_in.reshape(row_count // block_length, block_length, local_heads, head_dim)
    mixed_blocks = jnp.einsum("hij,njhc->nihc", position_mix, blocks, preferred_element_type=f32)
    mixed_blocks = mixed_blocks + position_bias.T[None, :, :, None]
    gated_mix = jax.nn.gelu(carry_branch, approximate=False) * mixed_blocks.reshape(row_count, width)
    blend_gate = jax.nn.sigmoid(jnp.dot(normed, blend_weight, preferred_element_type=f32))

    keys, gated_mix, blend_gate = lax.optimization_barrier((keys, gated_mix, blend_gate))
    value_shape = (owner_count, cap, head_dim, local_heads * span_length)
    level_shape = (owner_count, cap, local_heads * span_length)
    vmem = pl.BlockSpec(memory_space=pltpu.VMEM)
    back_values, back_levels = pl.pallas_call(
        functools.partial(attention_kernel, local_heads, owner_count, cap),
        in_specs=[pl.BlockSpec(memory_space=pltpu.SMEM)] * 2 + [vmem] * 3,
        out_specs=[vmem, vmem],
        out_shape=[jax.ShapeDtypeStruct(value_shape, bf16), jax.ShapeDtypeStruct(level_shape, f32)],
        scratch_shapes=[
            pltpu.VMEM(value_shape, bf16),
            pltpu.VMEM(level_shape, f32),
            pltpu.SemaphoreType.DMA((2, owner_count)),
            pltpu.SemaphoreType.DMA((2, owner_count)),
        ],
        compiler_params=pltpu.CompilerParams(collective_id=0, has_side_effects=True),
        name="attention",
    )(slot_local, slot_span, all_queries, keys, values_t)

    spans = 4 if span_count % 4 == 0 else 1
    mixed_rows = pl.pallas_call(
        functools.partial(merge_kernel, local_heads, spans, pick_count),
        grid_spec=pltpu.PrefetchScalarGridSpec(
            num_scalar_prefetch=1,
            grid=(span_count // spans,),
            in_specs=[
                pl.BlockSpec((slots, head_dim, local_heads * span_length), lambda i, _: (0, 0, 0)),
                pl.BlockSpec((slots, 1, local_heads * span_length), lambda i, _: (0, 0, 0)),
                pl.BlockSpec((spans * span_length, width), lambda i, _: (i, 0)),
                pl.BlockSpec((spans * span_length, width), lambda i, _: (i, 0)),
            ],
            out_specs=pl.BlockSpec((spans * span_length, width), lambda i, _: (i, 0)),
        ),
        out_shape=jax.ShapeDtypeStruct((row_count, width), bf16),
        name="merge",
    )(
        position,
        back_values.reshape(slots, head_dim, local_heads * span_length),
        back_levels.reshape(slots, 1, local_heads * span_length),
        gated_mix,
        blend_gate,
    )
    by_rows = lax.all_to_all(mixed_rows, "tp", split_axis=0, concat_axis=1, tiled=True)
    return jnp.dot(by_rows, output_weight, preferred_element_type=f32).astype(bf16)


def solution(mesh):
    in_specs = (
        P("st", None),
        P("st", None),
        P("st", None, None),
        P(),
        P(),
        P(None, "tp"),
        P(None, "tp"),
        P("tp"),
        P("tp", None, None),
        P("tp", None),
        P(None, "tp"),
        P(None, "tp"),
        P(None, "tp"),
        P(None, "tp"),
        P(),
    )
    out_specs = P(("st", "tp"), None)
    return jax.shard_map(
        per_device, mesh=mesh, in_specs=in_specs, out_specs=out_specs, check_vma=False
    )
```
